32 devices in a mesh: ep: 8 (over z, y), tp: 4 (over x, core).
Axes of the slice: x: 2, y: 2, z: 4, core: 2. Of those that a mesh axis runs over, the one named last changes fastest.
Arguments:
- tokens: bfloat16 [256, 2048], P('ep', 'tp'), may hold values from -33 to 33
- previous: bfloat16 [256, 2048], P('ep', 'tp'), may hold values from -6 to 6
- first_norm_gain: float32 [2048], replicated, may hold values from 0.1 to 1.9
- token_shift_share: float32 [5, 2048], replicated, may hold values from 0 to 1
- receptance_weight: bfloat16 [2048, 1024], P(None, 'tp'), may hold values from -0.125 to 0.125
- key_weight: bfloat16 [2048, 1024], P(None, 'tp'), may hold values from -0.125 to 0.125
- value_weight: bfloat16 [2048, 1024], P(None, 'tp'), may hold values from -0.125 to 0.125
- decay_down_map: bfloat16 [2048, 128], replicated, may hold values from -0.125 to 0.125
- decay_up_map: bfloat16 [128, 1024], replicated, may hold values from -0.5 to 0.5
- decay_offset: float32 [1024], P('tp'), may hold values from -4 to 1
- strength_down_map: bfloat16 [2048, 128], replicated, may hold values from -0.125 to 0.125
- strength_up_map: bfloat16 [128, 1024], replicated, may hold values from -0.5 to 0.5
- removal_key_scale: float32 [1024], P('tp'), may hold values from 0.3 to 3
- key_damping: float32 [1024], P('tp'), may hold values from 0.1 to 1.9
- self_term_weight: float32 [16, 64], P('tp'), may hold values from -0.6 to 0.6
- head_norm_gain: float32 [1024], P('tp'), may hold values from 0.1 to 1.9
- output_weight: bfloat16 [1024, 2048], P('tp'), may hold values from -0.1875 to 0.1875
- state: float32 [256, 16, 64, 64], P('ep', 'tp'), may hold values from -6 to 6
- second_norm_gain: float32 [2048], replicated, may hold values from 0.1 to 1.9
- routes: int32 [256, 4], P('ep'), may hold values from 0 to 7, all different within a row; in each aligned block of 32 rows (0 to 31, 32 to 63, ...) at most 24 rows name the same one
- chosen_expert_weight: float32 [256, 4], P('ep'), may hold values from 0.1 to 1
- expert_gate_weight: bfloat16 [8, 2048, 1024], P('ep', None, 'tp'), may hold values from -0.5 to 0.5
- expert_up_weight: bfloat16 [8, 2048, 1024], P('ep', None, 'tp'), may hold values from -0.5 to 0.5
- expert_down_weight: bfloat16 [8, 1024, 2048], P('ep', 'tp'), may hold values from -0.046875 to 0.046875
Outputs:
- layer_out: bfloat16 [256, 2048], P('ep', 'tp')
- new_state: float32 [256, 16, 64, 64], P('ep', 'tp')
The draws below stay inside these ranges and needn't reach their ends.
Inputs may be any that keep to these rules, and one draw needn't show every extreme that they name: `routes`: each row names 4 different experts. Among the rows of one index of ep no expert is named by more than 24 rows, and in every draw some expert is named by exactly 24 rows of some index of ep.
All inputs are finite; a program needn't handle non-finite values.
Results may differ from the reference program's by a relative error of at most 0.015.
Values may be sent and summed in bfloat16 or wider, within the bound.
A program may use at most 64 MiB of HBM per device.

```python
import math
import jax
import jax.numpy as jnp
import numpy as np
from jax import lax

D = 2048
HEAD_TOTAL = 16
HEAD_WIDTH = 64
DECAY_RANK = 128
ALPHA_RANK = 128
FF = 1024
TOP_K = 4
SEQ_DEV = 32
SEQS = 256
EXPERTS = 8
CAP = 24
N_EP = 8
N_TP = 4


def draw_tokens(key, part):
    row_key = jax.random.fold_in(key, 11)
    col_key = jax.random.fold_in(key, 12)
    base_key = jax.random.fold_in(key, 13)
    row_scales = jnp.exp(jax.random.uniform(row_key, (SEQS, 1), jnp.float32, -0.69, 0.69))
    ramp = jnp.exp((jnp.arange(D, dtype=jnp.float32) / D - 0.5) * 1.0986)
    col_scales = jnp.exp(jax.random.uniform(col_key, (1, D), jnp.float32, -1.15, 1.15)) * ramp[None, :]
    base = jnp.clip(jax.random.normal(base_key, (SEQS, D), jnp.float32), -3.0, 3.0)
    return (base * row_scales * col_scales).astype(jnp.bfloat16)


def block_levels(stream_key, extent, pieces, low, top_value):
    loudness, own = 1.0, jax.random.fold_in(stream_key, 6)
    for axis_at, shards_of in pieces:
        steps = jnp.exp(jax.random.uniform(jax.random.fold_in(own, axis_at), (shards_of,), jnp.float32, low / len(pieces), top_value / len(pieces)))
        loudness = loudness * jnp.repeat(steps, extent[axis_at] // shards_of).reshape([-1 if axis == axis_at else 1 for axis in range(len(extent))])
    return loudness


def assign_block(key, own, number, rows, count, top, reach, skew):
    order = jax.random.permutation(key, count)
    crowded, usual = portions_of(count, rows * top, reach, skew, True), portions_of(count, rows * top, reach, skew, False)
    places = jnp.arange(count)

    def named(tallies, turn):
        used = int((tallies > 0).sum())
        fixed = max(1, used // 4)
        passed = fixed + (places - fixed + turn * (used - fixed)) % max(1, count - fixed)
        return jnp.zeros((count,), jnp.int32).at[order[jnp.where(places < fixed, places, passed)]].set(jnp.asarray(tallies, jnp.int32))

    tallies = jnp.where(number % 4 == 0, named(crowded, number // 4), named(usual, number - number // 4 - 1))
    mixed = jax.random.permutation(jax.random.fold_in(own, 3), count)
    giver, sink = mixed[0:count // 2 * 2:2], mixed[1:count // 2 * 2:2]
    room = jnp.minimum(tallies[giver] - 1, reach - tallies[sink]) // 2
    room = jnp.where((giver == order[0]) | (sink == order[0]) | (tallies[sink] == 0), 0, jnp.maximum(room, 0))
    passed = jax.random.randint(jax.random.fold_in(own, 4), (count // 2,), 0, 1 << 20) % (room + 1)
    tallies = tallies.at[giver].add(-passed).at[sink].add(passed)
    labels = jnp.searchsorted(jnp.cumsum(tallies), jnp.arange(rows * top), side="right").astype(jnp.int32)
    table = labels.reshape(top, rows).T
    table = table[jax.random.permutation(jax.random.fold_in(own, 1), rows)]
    turn = jax.random.randint(jax.random.fold_in(own, 2), (rows, 1), 0, top)
    return jnp.take_along_axis(table, (jnp.arange(top)[None, :] + turn) % top, axis=1)


def portions_of(number_of, total, reach, slope, full):
    weights = [(1 << 20) // math.isqrt(grade ** slope) + 1 for grade in range(1, number_of + 1)]
    largest = reach if full else min(reach, max(-(-total // number_of), total * weights[0] // sum(weights)))
    least = 1 if total - largest >= number_of - 1 else 0
    holding, rest = [largest] + [least] * (number_of - 1), total - largest - least * (number_of - 1)
    while rest > 0:
        free = [i for i in range(1, number_of) if holding[i] < largest] or [i for i in range(1, number_of) if holding[i] < reach]
        mass, left = sum([weights[i] for i in free]), rest
        for i in free:
            extra = min(reach - holding[i], max(1, left * weights[i] // mass), rest)
            holding[i] = holding[i] + extra
            rest = rest - extra
    return np.array(holding)


def centred(key, shape, deviation, most, cuts=(), kind=jnp.bfloat16):
    result = jax.random.normal(key, shape, jnp.float32) * deviation
    if len(cuts) > 0:
        result = block_levels(key, shape, cuts, -0.22, 0.18) * result
    return jnp.clip(result, min=-most, max=most).astype(kind)


def setup_inputs(seed: int = 0) -> dict:
    key_list = jax.random.split(jax.random.key(seed), 25)
    tokens = draw_tokens(jax.random.fold_in(key_list[24], 71), 0)
    previous = centred(key_list[1], (SEQS, D), 1.0, 6.0, ((0, 8), (1, 4)))
    first_norm_gain = jnp.clip(1.0 + 0.18 * jax.random.normal(key_list[2], (D,), jnp.float32), 0.1, 1.9)
    token_shift_share = jnp.clip(jax.random.uniform(key_list[3], (5, D), jnp.float32, 0.0, 1.0), 0.0, 1.0)
    receptance_weight = centred(key_list[4], (D, HEAD_TOTAL * HEAD_WIDTH), D ** -0.5, 0.125, ((1, 4),))
    key_weight = centred(key_list[5], (D, HEAD_TOTAL * HEAD_WIDTH), D ** -0.5, 0.125, ((1, 4),))
    value_weight = centred(key_list[6], (D, HEAD_TOTAL * HEAD_WIDTH), D ** -0.5, 0.125, ((1, 4),))
    decay_down_map = centred(key_list[7], (D, DECAY_RANK), D ** -0.5, 0.125)
    decay_up_map = centred(key_list[8], (DECAY_RANK, HEAD_TOTAL * HEAD_WIDTH), DECAY_RANK ** -0.5, 0.5)
    decay_offset = jnp.clip(-4.0 + 5.0 * jax.random.uniform(key_list[9], (HEAD_TOTAL * HEAD_WIDTH,), jnp.float32) ** block_levels(key_list[9], (HEAD_TOTAL * HEAD_WIDTH,), ((0, 4),), -0.2, 0.2), -4.0, 1.0)
    strength_down_map = centred(key_list[10], (D, ALPHA_RANK), D ** -0.5, 0.125)
    strength_up_map = centred(key_list[11], (ALPHA_RANK, HEAD_TOTAL * HEAD_WIDTH), ALPHA_RANK ** -0.5, 0.5)
    removal_key_scale = jnp.clip(jnp.exp(math.log(3.0) - 2.3025851 * jax.random.uniform(key_list[12], (HEAD_TOTAL * HEAD_WIDTH,), jnp.float32) ** block_levels(key_list[12], (HEAD_TOTAL * HEAD_WIDTH,), ((0, 4),), -0.2, 0.2)), 0.3, 3.0)
    key_damping = jnp.clip(1.0 + 0.18 * jax.random.normal(key_list[13], (HEAD_TOTAL * HEAD_WIDTH,), jnp.float32), 0.1, 1.9)
    self_term_weight = centred(key_list[14], (HEAD_TOTAL, HEAD_WIDTH), 0.1, 0.6, ((0, 4),), jnp.float32)
    head_norm_gain = jnp.clip(1.0 + 0.18 * jax.random.normal(key_list[15], (HEAD_TOTAL * HEAD_WIDTH,), jnp.float32), 0.1, 1.9)
    output_weight = centred(key_list[16], (HEAD_TOTAL * HEAD_WIDTH, D), (HEAD_TOTAL * HEAD_WIDTH) ** -0.5, 0.1875, ((0, 4),))
    state = centred(key_list[17], (SEQS, HEAD_TOTAL, HEAD_WIDTH, HEAD_WIDTH), 1.0, 6.0, ((0, 8), (1, 4)), jnp.float32)
    second_norm_gain = jnp.clip(1.0 + 0.18 * jax.random.normal(key_list[18], (D,), jnp.float32), 0.1, 1.9)
    routes_keys = jax.random.split(jax.random.fold_in(key_list[19], 1), SEQS // SEQ_DEV)
    routes_turns = jax.random.permutation(jax.random.fold_in(key_list[19], 3), SEQS // SEQ_DEV)
    routes = jax.vmap(lambda own, number: assign_block(jax.random.fold_in(key_list[19], 2), own, number, SEQ_DEV, EXPERTS, TOP_K, CAP, 2))(routes_keys, routes_turns).reshape((SEQS, TOP_K))
    chosen_expert_weight = jnp.clip(jnp.exp(math.log(1.0) - 2.3025851 * jax.random.uniform(key_list[20], (SEQS, TOP_K), jnp.float32) ** block_levels(key_list[20], (SEQS, TOP_K), ((0, 8),), -0.2, 0.2)), 0.1, 1.0)
    expert_gate_weight = centred(key_list[21], (EXPERTS, D, FF), (D // 16) ** -0.5, 0.5, ((0, 8), (2, 4)))
    expert_up_weight = centred(key_list[22], (EXPERTS, D, FF), (D // 16) ** -0.5, 0.5, ((0, 8), (2, 4)))
    expert_down_weight = centred(key_list[23], (EXPERTS, FF, D), (16 * FF) ** -0.5, 0.046875, ((0, 8), (1, 4)))
    return {"tokens": tokens, "previous": previous, "first_norm_gain": first_norm_gain, "token_shift_share": token_shift_share, "receptance_weight": receptance_weight, "key_weight": key_weight, "value_weight": value_weight, "decay_down_map": decay_down_map, "decay_up_map": decay_up_map, "decay_offset": decay_offset, "strength_down_map": strength_down_map, "strength_up_map": strength_up_map, "removal_key_scale": removal_key_scale, "key_damping": key_damping, "self_term_weight": self_term_weight, "head_norm_gain": head_norm_gain, "output_weight": output_weight, "state": state, "second_norm_gain": second_norm_gain, "routes": routes, "chosen_expert_weight": chosen_expert_weight, "expert_gate_weight": expert_gate_weight, "expert_up_weight": expert_up_weight, "expert_down_weight": expert_down_weight}


NORM_EPS = 1e-06
GROUP_EPS = 0.00064
KEY_EPS = 1e-06
GATE_LIMIT = 7.0
GATE_SLOPE = 1.702

def row_rescale(values, gain):
    return values * lax.rsqrt(lax.optimization_barrier(jnp.mean(values * values, axis=-1, keepdims=True)) + NORM_EPS) * gain

def head_combiner(present_rows, prior_rows, first_norm_gain, token_shift_share, receptance_weight, key_weight, value_weight, decay_down_map, decay_up_map, decay_offset, strength_down_map, strength_up_map, removal_key_scale, key_damping, self_term_weight, head_norm_gain, state):
    sequence_count = present_rows.shape[0]
    head_number = state.shape[1]
    head_extent = state.shape[2]
    normed = row_rescale(present_rows.astype(jnp.float32), first_norm_gain)
    before = prior_rows.astype(jnp.float32)

    def shifted(role):
        return (normed + (before - normed) * token_shift_share[role]).astype(jnp.bfloat16)

    def project(inputs, weight):
        return jnp.dot(inputs, weight, preferred_element_type=jnp.float32)

    def by_heads(values):
        return values.reshape(sequence_count, head_number, head_extent)
    receptance_rows = by_heads(project(shifted(0), receptance_weight))
    key_rows = by_heads(project(shifted(1), key_weight))
    value_matrix = by_heads(project(shifted(2), value_weight))
    decay_low = jnp.tanh(project(shifted(3), decay_down_map)).astype(jnp.bfloat16)
    decay_pre = decay_offset + project(decay_low, decay_up_map)
    decay = by_heads(jnp.exp(-jnp.exp(-jax.nn.softplus(-decay_pre) - 0.5)))
    alpha_low = project(shifted(4), strength_down_map).astype(jnp.bfloat16)
    alpha = by_heads(jax.nn.sigmoid(project(alpha_low, strength_up_map)))
    removal = key_rows * removal_key_scale.reshape(head_number, head_extent)
    removal = removal * lax.rsqrt(lax.optimization_barrier(jnp.sum(removal * removal, axis=-1, keepdims=True)) + KEY_EPS)
    blended_rows = key_rows * (1.0 + (alpha - 1.0) * key_damping.reshape(head_number, head_extent))
    highest = lax.Precision.HIGHEST
    along = jnp.einsum('shij,shj->shi', state, removal, precision=highest)
    new_state = state * decay[:, :, None, :] - along[..., None] * (removal * alpha)[:, :, None, :] + value_matrix[..., None] * blended_rows[:, :, None, :]
    readout = jnp.einsum('shij,shj->shi', new_state, receptance_rows, precision=highest)
    centered = readout - lax.optimization_barrier(jnp.mean(readout, axis=-1, keepdims=True))
    variance = lax.optimization_barrier(jnp.mean(centered * centered, axis=-1, keepdims=True))
    heads_normalised = centered * lax.rsqrt(variance + GROUP_EPS) * head_norm_gain.reshape(head_number, head_extent)
    self_term = lax.optimization_barrier(jnp.sum(receptance_rows * blended_rows * self_term_weight, axis=-1, keepdims=True)) * value_matrix
    mixed_inputs = (heads_normalised + self_term).reshape(sequence_count, head_number * head_extent).astype(jnp.bfloat16)
    return (mixed_inputs, new_state)

def split_sum(left, right):
    block_rows = left.shape[1] // N_TP
    total = jnp.zeros((left.shape[0], right.shape[1]), jnp.float32)
    for block_index in range(N_TP):
        lower = block_index * block_rows
        product = jnp.dot(left[:, lower:lower + block_rows], right[lower:lower + block_rows], preferred_element_type=jnp.float32).astype(jnp.bfloat16)
        total = total + lax.optimization_barrier(product).astype(jnp.float32)
    return total

def reference(tokens, previous, first_norm_gain, token_shift_share, receptance_weight, key_weight, value_weight, decay_down_map, decay_up_map, decay_offset, strength_down_map, strength_up_map, removal_key_scale, key_damping, self_term_weight, head_norm_gain, output_weight, state, second_norm_gain, routes, chosen_expert_weight, expert_gate_weight, expert_up_weight, expert_down_weight):
    model_width = tokens.shape[1]

    def one_group(blocks):
        present_rows, prior_rows, state_tile = blocks
        return head_combiner(present_rows, prior_rows, first_norm_gain, token_shift_share, receptance_weight, key_weight, value_weight, decay_down_map, decay_up_map, decay_offset, strength_down_map, strength_up_map, removal_key_scale, key_damping, self_term_weight, head_norm_gain, state_tile)
    mixed_inputs, new_state = lax.map(one_group, (tokens.reshape(N_EP, SEQ_DEV, model_width), previous.reshape(N_EP, SEQ_DEV, model_width), state.reshape(N_EP, SEQ_DEV, HEAD_TOTAL, HEAD_WIDTH, HEAD_WIDTH)))
    mixed_inputs = mixed_inputs.reshape(SEQS, HEAD_TOTAL * HEAD_WIDTH)
    new_state = new_state.reshape(SEQS, HEAD_TOTAL, HEAD_WIDTH, HEAD_WIDTH)
    residual = tokens.astype(jnp.float32) + split_sum(mixed_inputs, output_weight)
    expert_in = row_rescale(residual, second_norm_gain).astype(jnp.bfloat16)
    grouped = routes.reshape(N_EP, SEQ_DEV * TOP_K)
    expert_ids = jnp.arange(EXPERTS, dtype=jnp.int32)
    onehot = (grouped[:, :, None] == expert_ids[None, None, :]).astype(jnp.int32)
    ranking = lax.optimization_barrier(jnp.sum((jnp.cumsum(onehot, axis=1) - onehot) * onehot, axis=2))
    source = jnp.arange(N_EP, dtype=jnp.int32)[:, None]
    slot_index = (grouped * (N_EP * CAP) + source * CAP + ranking).reshape(-1).astype(jnp.int32)
    owner = (jnp.arange(SEQS * TOP_K, dtype=jnp.int32) // TOP_K).astype(jnp.int32)
    buffer = jnp.zeros((EXPERTS * N_EP * CAP, model_width), jnp.bfloat16).at[slot_index].set(expert_in[owner])

    def one_expert(blocks):
        rows_in, gate_weight, up_weight, down_weight = blocks
        gate_pre = jnp.minimum(jnp.dot(rows_in, gate_weight, preferred_element_type=jnp.float32), GATE_LIMIT)
        up_pre = jnp.clip(jnp.dot(rows_in, up_weight, preferred_element_type=jnp.float32), -GATE_LIMIT, GATE_LIMIT)
        activation = ((up_pre + 1.0) * gate_pre * jax.nn.sigmoid(GATE_SLOPE * gate_pre)).astype(jnp.bfloat16)
        return split_sum(activation, down_weight).astype(jnp.bfloat16)
    expert_out = lax.map(one_expert, (buffer.reshape(EXPERTS, N_EP * CAP, model_width), expert_gate_weight, expert_up_weight, expert_down_weight))
    picked = expert_out.reshape(EXPERTS * N_EP * CAP, model_width)[slot_index].astype(jnp.float32)
    picked = picked.reshape(SEQS, TOP_K, model_width)
    layer_out = (residual + lax.optimization_barrier(jnp.sum(picked * chosen_expert_weight[:, :, None], axis=1))).astype(jnp.bfloat16)
    return (layer_out, new_state)
```

```python
import math

import jax
import jax.numpy as jnp
from jax import lax
from jax.experimental import pallas as pl
from jax.experimental.pallas import tpu as pltpu
from jax.sharding import PartitionSpec as P

NORM_EPS = 1e-06
GROUP_EPS = 0.00064
KEY_EPS = 1e-06
GATE_LIMIT = 7.0
GATE_SLOPE = 1.702
MESH = pl.DeviceIdType.MESH
F32 = jnp.float32
BF16 = jnp.bfloat16
VMEM = pl.BlockSpec(memory_space=pltpu.VMEM)
ANY = pl.BlockSpec(memory_space=pl.ANY)
HIGHEST = lax.Precision.HIGHEST


def dot(a, b):
    return jnp.dot(a, b, preferred_element_type=F32)


def group_sum(values, width):
    total = values.shape[1]
    row = lax.broadcasted_iota(jnp.int32, (total, total), 0) // width
    col = lax.broadcasted_iota(jnp.int32, (total, total), 1) // width
    ones = jnp.where(row == col, 1.0, 0.0).astype(F32)
    return jnp.dot(values, ones, preferred_element_type=F32, precision=HIGHEST)


def project_kernel(
    tokens, previous, gain, share, offset, removal_scale, damping, self_weight,
    rw, kw, vw, dd, sd, du, su,
    wv_out, dec_out, ra_out, bl_out, v_out, rv_out, sv_out,
    rwv, kwv, vwv, ddv, sdv, duv, suv, gathered,
    weight_sem, local_sem, send_sem, recv_sem,
):
    t = lax.axis_index("tp")
    parts = gathered.shape[1]
    own = tokens.shape[1]
    heads = wv_out.shape[0]
    width = dec_out.shape[2]
    cols = heads * width
    own_cols = pl.ds(pl.multiple_of(t * cols, cols), cols)
    pairs = (
        (rw, rwv), (kw, kwv), (vw, vwv), (dd, ddv), (sd, sdv),
        (du.at[:, own_cols], duv), (su.at[:, own_cols], suv),
    )
    loads = [pltpu.make_async_copy(a, b, weight_sem.at[i]) for i, (a, b) in enumerate(pairs)]
    barrier = pltpu.get_barrier_semaphore()
    for d in range(1, parts):
        pl.semaphore_signal(barrier, inc=1, device_id={"tp": t ^ d}, device_id_type=MESH)
    locals_ = [
        pltpu.make_async_copy(ref, gathered.at[i, t], local_sem.at[i])
        for i, ref in enumerate((tokens, previous))
    ]
    for copy in locals_ + loads:
        copy.start()
    pl.semaphore_wait(barrier, parts - 1)
    copies = []
    for i, ref in enumerate((tokens, previous)):
        for d in range(parts - 1, 0, -1):
            copy = pltpu.make_async_remote_copy(
                src_ref=ref, dst_ref=gathered.at[i, t],
                send_sem=send_sem.at[i, d], recv_sem=recv_sem.at[i, d],
                device_id={"tp": t ^ d}, device_id_type=MESH,
            )
            copy.start()
            copies.append(copy)
    for copy in locals_:
        copy.wait()
    for copy in copies:
        copy.wait()
    squares = 0.0
    for b in range(parts):
        x = gathered[0, b].astype(F32)
        squares = squares + jnp.sum(x * x, axis=-1, keepdims=True)
    scale = lax.rsqrt(squares / (parts * own) + NORM_EPS)
    for copy in loads:
        copy.wait()
    sums = [0.0] * 5
    for b in range(parts):
        span = slice(b * own, (b + 1) * own)
        normed = gathered[0, b].astype(F32) * scale * gain[:, span]
        change = gathered[1, b].astype(F32) - normed
        for m, weight in enumerate((rwv, kwv, vwv, ddv, sdv)):
            shifted = (normed + change * share[m : m + 1, span]).astype(BF16)
            sums[m] = sums[m] + dot(shifted, weight[span, :])
    receptance, key, value = sums[:3]
    decay_pre = offset[...] + dot(jnp.tanh(sums[3]).astype(BF16), duv[...])
    decay = jnp.exp(-math.exp(-0.5) * jax.nn.sigmoid(decay_pre))
    alpha = jax.nn.sigmoid(dot(sums[4].astype(BF16), suv[...]))
    removal = key * removal_scale[...]
    removal = removal * lax.rsqrt(group_sum(removal * removal, width) + KEY_EPS)
    blended = key * (1.0 + (alpha - 1.0) * damping[...])
    strength = removal * alpha
    probe = decay * receptance - group_sum(strength * receptance, width) * removal
    both = receptance * blended
    rv_out[...] = group_sum(both, width) * value
    sv_out[...] = group_sum(both * self_weight[...], width) * value
    for h in range(heads):
        span = slice(h * width, (h + 1) * width)
        wv_out[h] = jnp.concatenate([removal[:, span], probe[:, span]], axis=1)
        dec_out[h] = decay[:, span]
        ra_out[h] = strength[:, span]
        bl_out[h] = blended[:, span]
        v_out[h] = value[:, span]


def project(tokens, previous, gain, share, offset, removal_scale, damping, self_weight, rw, kw, vw, dd, sd, du, su, heads, width, parts):
    rows, own = tokens.shape
    full = parts * own
    cols = heads * width
    head_rows = jax.ShapeDtypeStruct((heads, rows, width), F32)
    flat = jax.ShapeDtypeStruct((rows, cols), F32)
    return pl.pallas_call(
        project_kernel,
        out_shape=[jax.ShapeDtypeStruct((heads, rows, 2 * width), F32)] + [head_rows] * 4 + [flat] * 2,
        in_specs=[VMEM] * 8 + [ANY] * 7,
        out_specs=[VMEM] * 7,
        scratch_shapes=[
            pltpu.VMEM((full, cols), BF16), pltpu.VMEM((full, cols), BF16), pltpu.VMEM((full, cols), BF16),
            pltpu.VMEM(dd.shape, BF16), pltpu.VMEM(sd.shape, BF16),
            pltpu.VMEM((du.shape[0], cols), BF16), pltpu.VMEM((su.shape[0], cols), BF16),
            pltpu.VMEM((2, parts, rows, own), BF16),
            pltpu.SemaphoreType.DMA((7,)),
            pltpu.SemaphoreType.DMA((2,)),
            pltpu.SemaphoreType.DMA((2, parts)),
            pltpu.SemaphoreType.DMA((2, parts)),
        ],
        compiler_params=pltpu.CompilerParams(collective_id=0, has_side_effects=True, vmem_limit_bytes=24 << 20),
        name="gather_project",
    )(tokens, previous, gain, share, offset, removal_scale, damping, self_weight, rw, kw, vw, dd, sd, du, su)


def state_kernel(state, wv, dec, ra, bl, v, rv, sv, gain, new_state, mixed):
    rows, heads, width, _ = state.shape
    wide = 3 * width
    row = lax.broadcasted_iota(jnp.int32, (wide, wide), 0) // width
    col = lax.broadcasted_iota(jnp.int32, (wide, wide), 1) // width
    ones = jnp.where(row == col, 1.0, 0.0).astype(BF16)
    i = lax.broadcasted_iota(jnp.int32, (width, width), 0)
    j = lax.broadcasted_iota(jnp.int32, (width, width), 1)
    eye = jnp.where(i == j, 1.0, 0.0).astype(F32)
    i = lax.broadcasted_iota(jnp.int32, (width, 2 * width), 0)
    j = lax.broadcasted_iota(jnp.int32, (width, 2 * width), 1)
    late = j == i + width
    pieces = []
    for h in range(heads):
        block = state[:, h]
        twice = jnp.concatenate([block, block], axis=2)
        products = (twice * wv[h][:, None, :]).astype(BF16)
        spread = (eye[None] * v[h][:, None, :]).astype(BF16)
        left = jnp.concatenate([products, spread], axis=2)
        total = dot(left.reshape(rows * width, wide), ones).reshape(rows, width, wide)
        along = total[:, :, :width]
        columns = total[:, :, 2 * width :]
        new_state[:, h] = block * dec[h][:, None, :] - along * ra[h][:, None, :] + columns * bl[h][:, None, :]
        picked = jnp.sum(jnp.where(late[None], total[:, :, : 2 * width], 0.0), axis=1)
        readout = picked[:, width:] + rv[:, h * width : (h + 1) * width]
        centered = readout - jnp.mean(readout, axis=-1, keepdims=True)
        variance = jnp.mean(centered * centered, axis=-1, keepdims=True)
        pieces.append(centered * lax.rsqrt(variance + GROUP_EPS))
    mixed[...] = jnp.concatenate(pieces, axis=1) * gain[...] + sv[...]


def update_state(state, wv, dec, ra, bl, v, rv, sv, gain):
    seqs, heads, width, _ = state.shape
    rows = 8
    cols = heads * width
    head_block = pl.BlockSpec((heads, rows, width), lambda s: (0, s, 0))
    flat_block = pl.BlockSpec((rows, cols), lambda s: (s, 0))
    state_block = pl.BlockSpec((rows, heads, width, width), lambda s: (s, 0, 0, 0))
    return pl.pallas_call(
        state_kernel,
        grid=(seqs // rows,),
        out_shape=[jax.ShapeDtypeStruct(state.shape, F32), jax.ShapeDtypeStruct((seqs, cols), F32)],
        in_specs=[
            state_block,
            pl.BlockSpec((heads, rows, 2 * width), lambda s: (0, s, 0)),
            head_block, head_block, head_block, head_block, flat_block, flat_block,
            pl.BlockSpec((1, cols), lambda s: (0, 0)),
        ],
        out_specs=[state_block, flat_block],
        compiler_params=pltpu.CompilerParams(vmem_limit_bytes=24 << 20),
        name="state_update",
    )(state, wv, dec, ra, bl, v, rv, sv, gain)


def repeat(count, body):
    if count <= 8:
        for d in range(count):
            body(d)
    else:
        lax.fori_loop(0, count, lambda d, c: (body(d), c)[1], 0)


def expert_kernel(
    mixed, tokens, gain, dispatch, combine, ow, gw, uw, dw,
    out,
    owv, gwv, uwv, dwv, terms, terms_in, residual, outgoing, arrived,
    down, partner_in, partner_last, cross_out, cross_in, shares, returned,
    weight_sem, terms_send, terms_recv, go_send, go_recv, own_sem,
    x_send, x_recv, p_send, p_recv, f_send, f_recv,
    h_send, h_recv, l_send, l_recv, c_send, c_recv, b_send, b_recv, back_sem,
):
    t = lax.axis_index("tp")
    e = lax.axis_index("ep")
    parts = arrived.shape[0]
    n = returned.shape[0]
    slots = returned.shape[1]
    own = tokens.shape[1]
    partner, cross = t ^ 1, t ^ 2

    def remote(src, dst, send, recv, where):
        return pltpu.make_async_remote_copy(
            src_ref=src, dst_ref=dst, send_sem=send, recv_sem=recv, device_id=where, device_id_type=MESH
        )

    def span(index, size):
        return pl.ds(pl.multiple_of(index * size, size), size)

    barrier = pltpu.get_barrier_semaphore()
    for d in range(1, parts):
        pl.semaphore_signal(barrier, inc=1, device_id={"tp": t ^ d}, device_id_type=MESH)
    repeat(n - 1, lambda d: pl.semaphore_signal(
        barrier, inc=1, device_id={"ep": lax.rem(e + 1 + d, n)}, device_id_type=MESH))
    loads = [
        pltpu.make_async_copy(a, b, weight_sem.at[i])
        for i, (a, b) in enumerate(((ow, owv), (gw.at[0], gwv), (uw.at[0], uwv), (dw.at[0], dwv)))
    ]
    for copy in loads:
        copy.start()

    rows_in = mixed[...].astype(BF16)
    loads[0].wait()
    for d in range(parts - 1, 0, -1):
        terms[d] = dot(rows_in, owv[:, span(t ^ d, own)]).astype(BF16)
    pl.semaphore_wait(barrier, parts - 1 + n - 1)
    sends = [
        remote(terms.at[d], terms_in.at[d], terms_send.at[d], terms_recv.at[d], {"tp": t ^ d})
        for d in range(parts - 1, 0, -1)
    ]
    for copy in sends:
        copy.start()
    total = tokens[...].astype(F32) + dot(rows_in, owv[:, span(t, own)]).astype(BF16).astype(F32)
    for copy in sends:
        copy.wait()
    for d in range(1, parts):
        total = total + terms_in[d].astype(F32)
    residual[...] = total
    outgoing[...] = dot(dispatch[...], total.astype(BF16)).astype(BF16)

    own_copy = pltpu.make_async_copy(outgoing.at[span(e, slots)], arrived.at[t, span(e, slots)], own_sem)
    own_copy.start()

    def go(d):
        where = lax.rem(e + d, n)
        return remote(outgoing.at[span(where, slots)], arrived.at[t, span(e, slots)], go_send.at[d], go_recv.at[d], {"ep": where})

    def source(d):
        return span(lax.rem(e + n - d, n), slots)

    def across(d):
        piece = arrived.at[t, source(d)]
        return remote(piece, piece, x_send.at[d], x_recv.at[d], {"tp": cross})

    def beside(d):
        piece = arrived.at[t, source(d)]
        return remote(piece, piece, p_send.at[d], p_recv.at[d], {"tp": partner})

    def forward(d):
        piece = arrived.at[cross, source(d)]
        return remote(piece, piece, f_send.at[d], f_recv.at[d], {"tp": partner})

    repeat(n - 1, lambda d: go(d + 1).start())
    own_copy.wait()
    across(0).start()
    beside(0).start()

    def pass_on(d):
        go(d + 1).wait_recv()
        across(d + 1).start()
        beside(d + 1).start()
        across(d).wait_recv()
        forward(d).start()

    repeat(n - 1, pass_on)
    across(n - 1).wait_recv()
    forward(n - 1).start()
    for copy in loads[1:]:
        copy.wait()

    def block_sums(block):
        x = arrived[block].astype(F32)
        scaled = (x * gain[:, span(block, own)]).astype(BF16)
        return (
            jnp.sum(x * x, axis=-1, keepdims=True),
            dot(scaled, gwv[span(block, own), :]),
            dot(scaled, uwv[span(block, own), :]),
        )

    def add(a, b):
        return tuple(x + y for x, y in zip(a, b))

    sums = add(block_sums(t), block_sums(cross))
    repeat(n, lambda d: beside(d).wait_recv())
    sums = add(sums, block_sums(partner))
    repeat(n, lambda d: forward(d).wait_recv())
    sums = add(sums, block_sums(t ^ 3))
    squares, gate_pre, up_pre = sums
    scale = lax.rsqrt(squares / (parts * own) + NORM_EPS)
    gate_pre = jnp.minimum(gate_pre * scale, GATE_LIMIT)
    up_pre = jnp.clip(up_pre * scale, -GATE_LIMIT, GATE_LIMIT)
    activation = ((up_pre + 1.0) * gate_pre * jax.nn.sigmoid(GATE_SLOPE * gate_pre)).astype(BF16)

    def target(d):
        return span(lax.rem(e + d, n), slots)

    def hand(d):
        return remote(down.at[3, target(d)], partner_in.at[target(d)], h_send.at[d], h_recv.at[d], {"tp": partner})

    def last(d):
        return remote(down.at[1, target(d)], partner_last.at[target(d)], l_send.at[d], l_recv.at[d], {"tp": partner})

    def crossing(d):
        return remote(cross_out.at[target(d)], cross_in.at[target(d)], c_send.at[d], c_recv.at[d], {"tp": cross})

    def back(d):
        return remote(shares.at[target(d)], returned.at[e], b_send.at[d], b_recv.at[d], {"ep": lax.rem(e + d, n)})

    down[3] = dot(activation, dwv[:, span(t ^ 3, own)]).astype(BF16)
    repeat(n, lambda d: hand(d).start())
    down[2] = dot(activation, dwv[:, span(cross, own)]).astype(BF16)

    def pair(d):
        hand(d).wait_recv()
        at = target(d)
        cross_out[at, :] = (down[2, at, :].astype(F32) + partner_in[at, :].astype(F32)).astype(BF16)
        crossing(d).start()

    order = [d % n for d in range(1, n + 1)]
    if n <= 8:
        for d in order:
            pair(d)
    else:
        repeat(n, lambda d: pair(lax.rem(d + 1, n)))
    down[1] = dot(activation, dwv[:, span(partner, own)]).astype(BF16)
    repeat(n, lambda d: last(d).start())
    down[0] = dot(activation, dwv[:, span(t, own)]).astype(BF16)

    def finish(d):
        last(d).wait_recv()
        crossing(d).wait_recv()
        at = target(d)
        shares[at, :] = (
            down[0, at, :].astype(F32) + partner_last[at, :].astype(F32) + cross_in[at, :].astype(F32)
        ).astype(BF16)

    def finish_remote(d):
        finish(d + 1)
        back(d + 1).start()

    repeat(n - 1, finish_remote)
    finish(0)
    own_back = pltpu.make_async_copy(shares.at[span(e, slots)], returned.at[e], back_sem)
    own_back.start()
    own_back.wait()

    def settle(d):
        go(d + 1).wait_send()
        back(d + 1).wait_send()
        back(d + 1).wait_recv()

    def settle_local(d):
        for copy in (across(d), beside(d), forward(d), hand(d), last(d), crossing(d)):
            copy.wait_send()

    repeat(n, settle_local)
    repeat(n - 1, settle)
    back_rows = returned[...].reshape(n * slots, own)
    weights = combine[...]
    high = weights.astype(BF16)
    low = (weights - high.astype(F32)).astype(BF16)
    out[...] = (residual[...] + (dot(high, back_rows) + dot(low, back_rows))).astype(BF16)


def experts_stage(mixed, tokens, gain, dispatch, combine, ow, gw, uw, dw, n, slots, parts):
    rows, own = tokens.shape
    total = n * slots
    dma = pltpu.SemaphoreType.DMA
    block = pltpu.VMEM((total, own), BF16)
    return pl.pallas_call(
        expert_kernel,
        out_shape=jax.ShapeDtypeStruct((rows, own), BF16),
        in_specs=[VMEM] * 5 + [ANY] * 4,
        out_specs=VMEM,
        scratch_shapes=[
            pltpu.VMEM(ow.shape, BF16), pltpu.VMEM(gw.shape[1:], BF16),
            pltpu.VMEM(uw.shape[1:], BF16), pltpu.VMEM(dw.shape[1:], BF16),
            pltpu.VMEM((parts, rows, own), BF16), pltpu.VMEM((parts, rows, own), BF16),
            pltpu.VMEM((rows, own), F32), block,
            pltpu.VMEM((parts, total, own), BF16), pltpu.VMEM((parts, total, own), BF16),
            block, block, block, block, block,
            pltpu.VMEM((n, slots, own), BF16),
            dma((4,)), dma((parts,)), dma((parts,)), dma((n,)), dma((n,)), dma,
        ] + [dma((n,))] * 14 + [dma],
        compiler_params=pltpu.CompilerParams(collective_id=1, has_side_effects=True, vmem_limit_bytes=44 << 20),
        name="experts",
    )(mixed, tokens, gain, dispatch, combine, ow, gw, uw, dw)


def shards(
    tokens, previous, first_norm_gain, token_shift_share, receptance_weight, key_weight, value_weight,
    decay_down_map, decay_up_map, decay_offset, strength_down_map, strength_up_map, removal_key_scale,
    key_damping, self_term_weight, head_norm_gain, output_weight, state, second_norm_gain, routes,
    chosen_expert_weight, expert_gate_weight, expert_up_weight, expert_down_weight,
):
    parts = lax.axis_size("tp")
    n = lax.axis_size("ep")
    heads, width = state.shape[1], state.shape[2]

    def flat(values):
        return values.reshape(1, -1)

    wv, dec, ra, bl, v, rv, sv = project(
        tokens, previous, flat(first_norm_gain), token_shift_share, flat(decay_offset),
        flat(removal_key_scale), flat(key_damping), flat(self_term_weight),
        receptance_weight, key_weight, value_weight, decay_down_map, strength_down_map,
        decay_up_map, strength_up_map, heads, width, parts,
    )
    new_state, mixed = update_state(state, wv, dec, ra, bl, v, rv, sv, flat(head_norm_gain))

    sequences, choices = routes.shape
    capacity = max(2, 3 * sequences * choices // (2 * n))
    slots = min(sequences, -(-capacity // 16) * 16)
    ids = jnp.arange(n, dtype=jnp.int32)
    chosen = routes[:, :, None] == ids[None, None, :]
    named = jnp.any(chosen, axis=1)
    weight = jnp.sum(jnp.where(chosen, chosen_expert_weight[:, :, None], 0.0), axis=1)
    if slots == sequences:
        rank = jnp.broadcast_to(jnp.arange(sequences, dtype=jnp.int32)[:, None], named.shape)
    else:
        rank = jnp.cumsum(named.astype(jnp.int32), axis=0) - 1
    placed = named[:, :, None] & (rank[:, :, None] == jnp.arange(slots, dtype=jnp.int32)[None, None, :])
    placed = placed.reshape(sequences, n * slots)
    dispatch = placed.T.astype(BF16)
    combine = jnp.where(placed, jnp.repeat(weight, slots, axis=1), 0.0)
    layer_out = experts_stage(
        mixed, tokens, flat(second_norm_gain), dispatch, combine,
        output_weight, expert_gate_weight, expert_up_weight, expert_down_weight, n, slots, parts,
    )
    return (layer_out, new_state)


def solution(mesh):
    in_specs = (
        P("ep", "tp"), P("ep", "tp"), P(), P(), P(None, "tp"), P(None, "tp"), P(None, "tp"), P(), P(),
        P("tp"), P(), P(), P("tp"), P("tp"), P("tp", None), P("tp"), P("tp", None),
        P("ep", "tp", None, None), P(), P("ep", None), P("ep", None),
        P("ep", None, "tp"), P("ep", None, "tp"), P("ep", "tp", None),
    )
    out_specs = (P("ep", "tp"), P("ep", "tp", None, None))
    return jax.shard_map(shards, mesh=mesh, in_specs=in_specs, out_specs=out_specs, check_vma=False)
```

```python
import math

import jax
import jax.numpy as jnp
from jax import lax
from jax.experimental import pallas as pl
from jax.experimental.pallas import tpu as pltpu
from jax.sharding import PartitionSpec as P

NORM_EPS = 1e-06
GROUP_EPS = 0.00064
KEY_EPS = 1e-06
GATE_LIMIT = 7.0
GATE_SLOPE = 1.702
MESH = pl.DeviceIdType.MESH
F32 = jnp.float32
BF16 = jnp.bfloat16
VMEM = pl.BlockSpec(memory_space=pltpu.VMEM)
HBM = pl.BlockSpec(memory_space=pltpu.MemorySpace.HBM)
HIGHEST = lax.Precision.HIGHEST


def dot(a, b):
    return jnp.dot(a, b, preferred_element_type=F32)


def group_sum(values, width):
    total = values.shape[1]
    row = lax.broadcasted_iota(jnp.int32, (total, total), 0) // width
    col = lax.broadcasted_iota(jnp.int32, (total, total), 1) // width
    ones = jnp.where(row == col, 1.0, 0.0).astype(F32)
    return jnp.dot(values, ones, preferred_element_type=F32, precision=HIGHEST)


def project_kernel(
    tokens, previous, gain_in, share_in, offset_in, removal_in, damping_in, self_in,
    rw, kw, vw, dd, sd, du, su,
    wv_out, dec_out, ra_out, bl_out, v_out, rv_out, sv_out,
    gain, share, offset, removal_scale, damping, self_rows,
    rwv, kwv, vwv, ddv, sdv, duv, suv, gathered,
    weight_sem, local_sem, send_sem, recv_sem,
):
    t = lax.axis_index("tp")
    parts = gathered.shape[1]
    own = tokens.shape[1]
    heads = wv_out.shape[0]
    width = dec_out.shape[2]
    cols = heads * width
    own_cols = pl.ds(pl.multiple_of(t * cols, cols), cols)
    pairs = (
        (gain_in, gain), (share_in, share),
        (rw, rwv), (kw, kwv), (vw, vwv), (dd, ddv), (sd, sdv),
        (du.at[:, own_cols], duv), (su.at[:, own_cols], suv),
        (offset_in, offset), (removal_in, removal_scale), (damping_in, damping), (self_in, self_rows),
    )
    loads = [pltpu.make_async_copy(a, b, weight_sem.at[i]) for i, (a, b) in enumerate(pairs)]
    barrier = pltpu.get_barrier_semaphore()
    for d in range(1, parts):
        pl.semaphore_signal(barrier, inc=1, device_id={"tp": t ^ d}, device_id_type=MESH)
    locals_ = [
        pltpu.make_async_copy(ref, gathered.at[i, t], local_sem.at[i])
        for i, ref in enumerate((tokens, previous))
    ]
    for copy in locals_ + loads:
        copy.start()
    pl.semaphore_wait(barrier, parts - 1)
    copies = []
    for i in range(2):
        locals_[i].wait()
        for d in range(parts - 1, 0, -1):
            copy = pltpu.make_async_remote_copy(
                src_ref=gathered.at[i, t], dst_ref=gathered.at[i, t],
                send_sem=send_sem.at[i, d], recv_sem=recv_sem.at[i, d],
                device_id={"tp": t ^ d}, device_id_type=MESH,
            )
            copy.start()
            copies.append(copy)
    for copy in copies:
        copy.wait()
    squares = 0.0
    for b in range(parts):
        x = gathered[0, b].astype(F32)
        squares = squares + jnp.sum(x * x, axis=-1, keepdims=True)
    scale = lax.rsqrt(squares / (parts * own) + NORM_EPS)
    for copy in loads:
        copy.wait()
    sums = [0.0] * 5
    for b in range(parts):
        span = slice(b * own, (b + 1) * own)
        normed = gathered[0, b].astype(F32) * scale * gain[:, span]
        change = gathered[1, b].astype(F32) - normed
        for m, weight in enumerate((rwv, kwv, vwv, ddv, sdv)):
            shifted = (normed + change * share[m : m + 1, span]).astype(BF16)
            sums[m] = sums[m] + dot(shifted, weight[span, :])
    receptance, key, value = sums[:3]
    decay_pre = offset[...] + dot(jnp.tanh(sums[3]).astype(BF16), duv[...])
    decay = jnp.exp(-math.exp(-0.5) * jax.nn.sigmoid(decay_pre))
    alpha = jax.nn.sigmoid(dot(sums[4].astype(BF16), suv[...]))
    removal = key * removal_scale[...]
    removal = removal * lax.rsqrt(group_sum(removal * removal, width) + KEY_EPS)
    blended = key * (1.0 + (alpha - 1.0) * damping[...])
    strength = removal * alpha
    probe = decay * receptance - group_sum(strength * receptance, width) * removal
    both = receptance * blended
    self_weight = jnp.concatenate([self_rows[h : h + 1, :] for h in range(heads)], axis=1)
    rv_out[...] = group_sum(both, width) * value
    sv_out[...] = group_sum(both * self_weight, width) * value
    for h in range(heads):
        span = slice(h * width, (h + 1) * width)
        wv_out[h] = jnp.concatenate([removal[:, span], probe[:, span]], axis=1)
        dec_out[h] = decay[:, span]
        ra_out[h] = strength[:, span]
        bl_out[h] = blended[:, span]
        v_out[h] = value[:, span]


def project(tokens, previous, gain, share, offset, removal_scale, damping, self_weight, rw, kw, vw, dd, sd, du, su, heads, width, parts):
    rows, own = tokens.shape
    full = parts * own
    cols = heads * width
    head_rows = jax.ShapeDtypeStruct((heads, rows, width), F32)
    flat = jax.ShapeDtypeStruct((rows, cols), F32)
    return pl.pallas_call(
        project_kernel,
        out_shape=[jax.ShapeDtypeStruct((heads, rows, 2 * width), F32)] + [head_rows] * 4 + [flat] * 2,
        in_specs=[HBM] * 15,
        out_specs=[VMEM] * 7,
        scratch_shapes=[
            pltpu.VMEM(gain.shape, F32), pltpu.VMEM(share.shape, F32), pltpu.VMEM(offset.shape, F32),
            pltpu.VMEM(removal_scale.shape, F32), pltpu.VMEM(damping.shape, F32), pltpu.VMEM(self_weight.shape, F32),
            pltpu.VMEM((full, cols), BF16), pltpu.VMEM((full, cols), BF16), pltpu.VMEM((full, cols), BF16),
            pltpu.VMEM(dd.shape, BF16), pltpu.VMEM(sd.shape, BF16),
            pltpu.VMEM((du.shape[0], cols), BF16), pltpu.VMEM((su.shape[0], cols), BF16),
            pltpu.VMEM((2, parts, rows, own), BF16),
            pltpu.SemaphoreType.DMA((13,)),
            pltpu.SemaphoreType.DMA((2,)),
            pltpu.SemaphoreType.DMA((2, parts)),
            pltpu.SemaphoreType.DMA((2, parts)),
        ],
        compiler_params=pltpu.CompilerParams(collective_id=0, has_side_effects=True, vmem_limit_bytes=67_000_000),
        name="gather_project",
    )(tokens, previous, gain, share, offset, removal_scale, damping, self_weight, rw, kw, vw, dd, sd, du, su)


def state_kernel(state, wv, dec, ra, bl, v, rv, sv, gain, new_state, mixed):
    rows, heads, width, _ = state.shape
    wide = 3 * width
    row = lax.broadcasted_iota(jnp.int32, (wide, wide), 0) // width
    col = lax.broadcasted_iota(jnp.int32, (wide, wide), 1) // width
    ones = jnp.where(row == col, 1.0, 0.0).astype(BF16)
    i = lax.broadcasted_iota(jnp.int32, (width, width), 0)
    j = lax.broadcasted_iota(jnp.int32, (width, width), 1)
    eye = jnp.where(i == j, 1.0, 0.0).astype(F32)
    i = lax.broadcasted_iota(jnp.int32, (width, 2 * width), 0)
    j = lax.broadcasted_iota(jnp.int32, (width, 2 * width), 1)
    late = j == i + width
    pieces = []
    for h in range(heads):
        block = state[:, h]
        twice = jnp.concatenate([block, block], axis=2)
        products = (twice * wv[h][:, None, :]).astype(BF16)
        spread = (eye[None] * v[h][:, None, :]).astype(BF16)
        left = jnp.concatenate([products, spread], axis=2)
        total = dot(left.reshape(rows * width, wide), ones).reshape(rows, width, wide)
        along = total[:, :, :width]
        columns = total[:, :, 2 * width :]
        new_state[:, h] = block * dec[h][:, None, :] - along * ra[h][:, None, :] + columns * bl[h][:, None, :]
        picked = jnp.sum(jnp.where(late[None], total[:, :, : 2 * width], 0.0), axis=1)
        readout = picked[:, width:] + rv[:, h * width : (h + 1) * width]
        centered = readout - jnp.mean(readout, axis=-1, keepdims=True)
        variance = jnp.mean(centered * centered, axis=-1, keepdims=True)
        pieces.append(centered * lax.rsqrt(variance + GROUP_EPS))
    mixed[...] = jnp.concatenate(pieces, axis=1) * gain[...] + sv[...]


def update_state(state, wv, dec, ra, bl, v, rv, sv, gain):
    seqs, heads, width, _ = state.shape
    rows = 8
    cols = heads * width
    head_block = pl.BlockSpec((heads, rows, width), lambda s: (0, s, 0))
    flat_block = pl.BlockSpec((rows, cols), lambda s: (s, 0))
    state_block = pl.BlockSpec((rows, heads, width, width), lambda s: (s, 0, 0, 0))
    return pl.pallas_call(
        state_kernel,
        grid=(seqs // rows,),
        out_shape=[jax.ShapeDtypeStruct(state.shape, F32), jax.ShapeDtypeStruct((seqs, cols), F32)],
        in_specs=[
            state_block,
            pl.BlockSpec((heads, rows, 2 * width), lambda s: (0, s, 0)),
            head_block, head_block, head_block, head_block, flat_block, flat_block,
            pl.BlockSpec((1, cols), lambda s: (0, 0)),
        ],
        out_specs=[state_block, flat_block],
        compiler_params=pltpu.CompilerParams(vmem_limit_bytes=67_000_000),
        name="state_update",
    )(state, wv, dec, ra, bl, v, rv, sv, gain)


def repeat(first, end, body):
    if end - first <= 8:
        for d in range(first, end):
            body(d)
    else:
        lax.fori_loop(first, end, lambda d, c: (body(d), c)[1], 0)


def expert_kernel(
    mixed_in, tokens_in, gain_in, routes_in, chosen_in, ow_in, gw, uw, dw,
    out,
    mixed, tokens, gain, routes, chosen, ow, gwv, uwv, dwv, terms, terms_in, residual, outgoing, arrived,
    down, partner_in, partner_last, cross_out, cross_in, shares, returned, combine,
    weight_sem, terms_send, terms_recv, own_sem,
    go_send, go_recv, x_send, x_recv, p_send, p_recv, f_send, f_recv,
    h_send, h_recv, l_send, l_recv, c_send, c_recv, b_send, b_recv,
):
    t = lax.axis_index("tp")
    e = lax.axis_index("ep")
    parts = arrived.shape[0]
    n = go_send.shape[0]
    total_slots, own = returned.shape
    slots = total_slots // n
    seqs = tokens.shape[0]
    dense = slots == seqs
    partner, cross = t ^ 1, t ^ 2

    def remote(src, dst, send, recv, where):
        return pltpu.make_async_remote_copy(
            src_ref=src, dst_ref=dst, send_sem=send, recv_sem=recv, device_id=where, device_id_type=MESH
        )

    def span(index, size):
        if isinstance(index, int):
            return pl.ds(index * size, size)
        return pl.ds(pl.multiple_of(index * size, size), size)

    barrier = pltpu.get_barrier_semaphore()
    for d in range(1, parts):
        pl.semaphore_signal(barrier, inc=1, device_id={"tp": t ^ d}, device_id_type=MESH)
    repeat(1, n, lambda d: pl.semaphore_signal(
        barrier, inc=1, device_id={"ep": lax.rem(e + d, n)}, device_id_type=MESH))
    loads = [
        pltpu.make_async_copy(a, b, weight_sem.at[i])
        for i, (a, b) in enumerate((
            (mixed_in, mixed), (ow_in, ow), (tokens_in, tokens), (routes_in, routes), (chosen_in, chosen),
            (gain_in, gain), (gw.at[0], gwv), (uw.at[0], uwv), (dw.at[0], dwv),
        ))
    ]
    for copy in loads:
        copy.start()

    for copy in loads[:5]:
        copy.wait()
    rows_in = mixed[...].astype(BF16)
    for d in range(parts - 1, 0, -1):
        terms[d] = dot(rows_in, ow[:, span(t ^ d, own)]).astype(BF16)
    pl.semaphore_wait(barrier, parts - 1 + n - 1)
    sends = [
        remote(terms.at[d], terms_in.at[d], terms_send.at[d], terms_recv.at[d], {"tp": t ^ d})
        for d in range(parts - 1, 0, -1)
    ]
    for copy in sends:
        copy.start()
    total = tokens[...].astype(F32) + dot(rows_in, ow[:, span(t, own)]).astype(BF16).astype(F32)

    column = lax.broadcasted_iota(jnp.int32, (total_slots, seqs), 0)
    sequence = lax.broadcasted_iota(jnp.int32, (total_slots, seqs), 1)
    expert = lax.rem(e + column // slots, n)
    weight = jnp.zeros((total_slots, seqs), F32)
    named = jnp.zeros((total_slots, seqs), F32)
    for k in range(routes.shape[0]):
        hit = routes[k : k + 1, :] == expert
        weight = weight + jnp.where(hit, chosen[k : k + 1, :], 0.0)
        named = named + jnp.where(hit, 1.0, 0.0)
    if dense:
        placed = jnp.where(sequence == column % slots, named, 0.0)
    else:
        i = lax.broadcasted_iota(jnp.int32, (seqs, seqs), 0)
        j = lax.broadcasted_iota(jnp.int32, (seqs, seqs), 1)
        before = jnp.where(i < j, 1.0, 0.0).astype(BF16)
        rank = dot(named.astype(BF16), before)
        placed = jnp.where(rank == (column % slots).astype(F32), named, 0.0)
    combine[...] = (placed * weight).T

    for copy in sends:
        copy.wait()
    for d in range(1, parts):
        total = total + terms_in[d].astype(F32)
    residual[...] = total
    if dense:
        outgoing[...] = total.astype(BF16)
    else:
        outgoing[...] = dot(placed.astype(BF16), total.astype(BF16)).astype(BF16)

    def outgoing_block(d):
        return outgoing if dense else outgoing.at[span(d, slots)]

    def go(d):
        return remote(
            outgoing_block(d), arrived.at[t, span(d, slots)], go_send.at[d], go_recv.at[d],
            {"ep": lax.rem(e + d, n)},
        )

    def across(d):
        piece = arrived.at[t, span(d, slots)]
        return remote(piece, piece, x_send.at[d], x_recv.at[d], {"tp": cross})

    def beside(d):
        piece = arrived.at[t, span(d, slots)]
        return remote(piece, piece, p_send.at[d], p_recv.at[d], {"tp": partner})

    def forward(d):
        piece = arrived.at[cross, span(d, slots)]
        return remote(piece, piece, f_send.at[d], f_recv.at[d], {"tp": partner})

    def hand(d):
        at = span(d, slots)
        return remote(down.at[3, at], partner_in.at[at], h_send.at[d], h_recv.at[d], {"tp": partner})

    def last(d):
        at = span(d, slots)
        return remote(down.at[1, at], partner_last.at[at], l_send.at[d], l_recv.at[d], {"tp": partner})

    def crossing(d):
        at = span(d, slots)
        return remote(cross_out.at[at], cross_in.at[at], c_send.at[d], c_recv.at[d], {"tp": cross})

    def back(d):
        at = span(d, slots)
        return remote(shares.at[at], returned.at[at], b_send.at[d], b_recv.at[d], {"ep": lax.rem(e + n - d, n)})

    def spread(d):
        across(d).start()
        beside(d).start()

    def pass_on(d):
        across(d).wait_recv()
        forward(d).start()

    def arrive(first, end):
        def one(d):
            go(d).wait_recv()
            spread(d)
            pass_on(d - 1)

        repeat(max(first, 1), end, one)

    def block_sums(block, rows):
        x = arrived[block, rows, :].astype(F32)
        scaled = (x * gain[:, span(block, own)]).astype(BF16)
        return (
            jnp.sum(x * x, axis=-1, keepdims=True),
            dot(scaled, gwv[span(block, own), :]),
            dot(scaled, uwv[span(block, own), :]),
        )

    def add(a, b):
        return tuple(x + y for x, y in zip(a, b))

    def expert_rows(first, end):
        rows = pl.ds(first * slots, (end - first) * slots)
        sums = add(block_sums(t, rows), block_sums(cross, rows))
        repeat(first, end, lambda d: beside(d).wait_recv())
        sums = add(sums, block_sums(partner, rows))
        repeat(first, end, lambda d: forward(d).wait_recv())
        squares, gate_pre, up_pre = add(sums, block_sums(t ^ 3, rows))
        scale = lax.rsqrt(squares / (parts * own) + NORM_EPS)
        gate_pre = jnp.minimum(gate_pre * scale, GATE_LIMIT)
        up_pre = jnp.clip(up_pre * scale, -GATE_LIMIT, GATE_LIMIT)
        activation = ((up_pre + 1.0) * gate_pre * jax.nn.sigmoid(GATE_SLOPE * gate_pre)).astype(BF16)
        down[3, rows, :] = dot(activation, dwv[:, span(t ^ 3, own)]).astype(BF16)
        repeat(first, end, lambda d: hand(d).start())
        down[2, rows, :] = dot(activation, dwv[:, span(cross, own)]).astype(BF16)
        down[1, rows, :] = dot(activation, dwv[:, span(partner, own)]).astype(BF16)
        repeat(first, end, lambda d: last(d).start())
        down[0, rows, :] = dot(activation, dwv[:, span(t, own)]).astype(BF16)

    def pair(d):
        hand(d).wait_recv()
        at = span(d, slots)
        cross_out[at, :] = (down[2, at, :].astype(F32) + partner_in[at, :].astype(F32)).astype(BF16)
        crossing(d).start()

    def finish(d):
        last(d).wait_recv()
        crossing(d).wait_recv()
        at = span(d, slots)
        return (
            down[0, at, :].astype(F32) + partner_last[at, :].astype(F32) + cross_in[at, :].astype(F32)
        ).astype(BF16)

    def send_back(d):
        shares[span(d, slots), :] = finish(d)
        back(d).start()

    own_copy = pltpu.make_async_copy(outgoing_block(0), arrived.at[t, span(0, slots)], own_sem)
    own_copy.start()
    repeat(1, n, lambda d: go(d).start())
    own_copy.wait()
    spread(0)
    half = n // 2
    arrive(0, half)
    pass_on(half - 1)
    for copy in loads[5:]:
        copy.wait()
    expert_rows(0, half)

    def arrive_first(d):
        go(d).wait_recv()
        spread(d)

    arrive_first(half)
    repeat(0, half, pair)
    arrive(half + 1, n)
    pass_on(n - 1)
    repeat(1, half, send_back)
    expert_rows(half, n)
    repeat(half, n, pair)
    returned[pl.ds(0, slots), :] = finish(0)
    repeat(half, n, send_back)

    def settle(d):
        go(d).wait_send()
        back(d).wait_send()

    def settle_local(d):
        for copy in (across(d), beside(d), forward(d), hand(d), last(d), crossing(d)):
            copy.wait_send()

    repeat(0, n, settle_local)
    repeat(1, n, settle)
    weights = combine[...]
    high = weights.astype(BF16)
    low = (weights - high.astype(F32)).astype(BF16)
    repeat(1, n, lambda d: back(d).wait_recv())
    rows_back = returned[...]
    out[...] = (residual[...] + (dot(high, rows_back) + dot(low, rows_back))).astype(BF16)


def experts_stage(mixed, tokens, gain, routes, chosen, ow, gw, uw, dw, n, slots, parts):
    rows, own = tokens.shape
    total = n * slots
    dma = pltpu.SemaphoreType.DMA
    block = pltpu.VMEM((total, own), BF16)
    return pl.pallas_call(
        expert_kernel,
        out_shape=jax.ShapeDtypeStruct((rows, own), BF16),
        in_specs=[HBM] * 9,
        out_specs=VMEM,
        scratch_shapes=[
            pltpu.VMEM(mixed.shape, F32), pltpu.VMEM(tokens.shape, BF16), pltpu.VMEM(gain.shape, F32),
            pltpu.VMEM(routes.shape, jnp.int32), pltpu.VMEM(chosen.shape, F32), pltpu.VMEM(ow.shape, BF16),
            pltpu.VMEM(gw.shape[1:], BF16), pltpu.VMEM(uw.shape[1:], BF16), pltpu.VMEM(dw.shape[1:], BF16),
            pltpu.VMEM((parts, rows, own), BF16), pltpu.VMEM((parts, rows, own), BF16),
            pltpu.VMEM((rows, own), F32),
            pltpu.VMEM((rows if slots == rows else total, own), BF16),
            pltpu.VMEM((parts, total, own), BF16), pltpu.VMEM((parts, total, own), BF16),
            block, block, block, block, block, block,
            pltpu.VMEM((rows, total), F32),
            dma((9,)), dma((parts,)), dma((parts,)), dma,
        ] + [dma((n,))] * 16,
        compiler_params=pltpu.CompilerParams(collective_id=1, has_side_effects=True, vmem_limit_bytes=67_000_000),
        name="experts",
    )(mixed, tokens, gain, routes, chosen, ow, gw, uw, dw)


def shards(
    tokens, previous, first_norm_gain, token_shift_share, receptance_weight, key_weight, value_weight,
    decay_down_map, decay_up_map, decay_offset, strength_down_map, strength_up_map, removal_key_scale,
    key_damping, self_term_weight, head_norm_gain, output_weight, state, second_norm_gain, routes,
    chosen_expert_weight, expert_gate_weight, expert_up_weight, expert_down_weight,
):
    parts = lax.axis_size("tp")
    n = lax.axis_size("ep")
    heads, width = state.shape[1], state.shape[2]

    def flat(values):
        return values.reshape(1, -1)

    wv, dec, ra, bl, v, rv, sv = project(
        tokens, previous, flat(first_norm_gain), token_shift_share, flat(decay_offset),
        flat(removal_key_scale), flat(key_damping), self_term_weight,
        receptance_weight, key_weight, value_weight, decay_down_map, strength_down_map,
        decay_up_map, strength_up_map, heads, width, parts,
    )
    new_state, mixed = update_state(state, wv, dec, ra, bl, v, rv, sv, flat(head_norm_gain))

    sequences, choices = routes.shape
    capacity = max(2, 3 * sequences * choices // (2 * n))
    slots = min(sequences, -(-capacity // 16) * 16)
    layer_out = experts_stage(
        mixed, tokens, flat(second_norm_gain), routes.T, chosen_expert_weight.T,
        output_weight, expert_gate_weight, expert_up_weight, expert_down_weight, n, slots, parts,
    )
    return (layer_out, new_state)


def solution(mesh):
    in_specs = (
        P("ep", "tp"), P("ep", "tp"), P(), P(), P(None, "tp"), P(None, "tp"), P(None, "tp"), P(), P(),
        P("tp"), P(), P(), P("tp"), P("tp"), P("tp", None), P("tp"), P("tp", None),
        P("ep", "tp", None, None), P(), P("ep", None), P("ep", None),
        P("ep", None, "tp"), P("ep", None, "tp"), P("ep", "tp", None),
    )
    out_specs = (P("ep", "tp"), P("ep", "tp", None, None))
    return jax.shard_map(shards, mesh=mesh, in_specs=in_specs, out_specs=out_specs, check_vma=False)
```
